32 devices in a mesh: ep: 32 (over z, y, x, core).
Axes of the slice: x: 2, y: 2, z: 4, core: 2. Of those that a mesh axis runs over, the one named last changes fastest.
Arguments:
- tokens: bfloat16 [1024, 2048], P('ep'), may hold values from -6 to 6
- gain_mix: float32 [2048], replicated, may hold values from 0.1 to 1.9
- w_query: bfloat16 [2048, 384], replicated, may hold values from -0.125 to 0.125
- w_key: bfloat16 [2048, 384], replicated, may hold values from -0.125 to 0.125
- w_value: bfloat16 [2048, 768], replicated, may hold values from -0.125 to 0.125
- w_input_gate: bfloat16 [2048, 4], replicated, may hold values from -0.125 to 0.125
- w_forget_gate: bfloat16 [2048, 4], replicated, may hold values from -0.125 to 0.125
- bias_input: float32 [4], replicated, may hold values from -1 to 1
- bias_forget: float32 [4], replicated, may hold values from 0 to 5
- memory_cells: float32 [1024, 4, 96, 192], P('ep'), may hold values from -6 to 6
- normalizer: float32 [1024, 4, 96], P('ep'), may hold values from -6 to 6
- stabilizer: float32 [1024, 4], P('ep'), may hold values from -1 to 1
- w_mix_out: bfloat16 [768, 2048], replicated, may hold values from -0.21875 to 0.21875
- gain_mix_post: float32 [2048], replicated, may hold values from 0.1 to 1.9
- gain_ffn: float32 [2048], replicated, may hold values from 0.1 to 1.9
- w_router: bfloat16 [2048, 8], replicated, may hold values from -0.125 to 0.125
- routing: int32 [1024, 2], replicated, may hold values from 0 to 7, all different within a row; in each aligned block of 32 rows (0 to 31, 32 to 63, ...) at most 16 rows name the same one
- w_expert_gate: bfloat16 [32, 2048, 384], P('ep'), may hold values from -0.125 to 0.125
- w_expert_up: bfloat16 [32, 2048, 384], P('ep'), may hold values from -0.125 to 0.125
- w_expert_down: bfloat16 [32, 384, 2048], P('ep'), may hold values from -0.15625 to 0.15625
- gain_ffn_post: float32 [2048], replicated, may hold values from 0.1 to 1.9
Outputs:
- mixed: bfloat16 [1024, 2048], P('ep')
- cells_next: float32 [1024, 4, 96, 192], P('ep')
- normalizer_next: float32 [1024, 4, 96], P('ep')
- stabilizer_next: float32 [1024, 4], P('ep')
The draws below stay inside these ranges and needn't reach their ends.
Inputs may be any that keep to these rules, and one draw needn't show every extreme that they name: `routing`: each row names 2 different experts. In the rows of one device (aligned blocks of 32 rows) no expert is named more than 16 times, a bound that some block reaches.
All inputs are finite; a program needn't handle non-finite values.
Results may differ from the reference program's by a relative error of at most 0.012.
Values may be sent and summed in bfloat16 or wider, within the bound.
A program may use at most 128 MiB of HBM per device.

```python
import math
import jax
import jax.numpy as jnp
import numpy as np
from jax import lax

D = 2048
HEADS = 4
DK = 96
DV = 192
FF_E = 1536
SPLIT = 4
TOP_K = 2
SEQ_DEV = 32
EXPERTS = 8
CAP = 16
TOKENS = 1024
N_EP = 32


def block_levels(stream_key, dims, split, smallest, largest):
    factor_of = 1.0
    for dim, parts in split:
        steps = jax.random.uniform(jax.random.fold_in(jax.random.fold_in(stream_key, 6), dim), (parts,), jnp.float32, smallest / len(split), largest / len(split))
        factor_of = factor_of * jnp.repeat(jnp.exp(steps), dims[dim] // parts).reshape((-1,) + (1,) * (len(dims) - 1 - dim))
    return factor_of


def routed_block(rng, own, number, rows, number_of, top, bound, lean):
    sequence = jax.random.permutation(rng, number_of)
    heavy_load, ordinary = shares(number_of, rows * top, bound, lean, True), shares(number_of, rows * top, bound, lean, False)
    places = jnp.arange(number_of)

    def named(tallies, offset_by):
        used = int((tallies > 0).sum())
        fixed = max(1, used // 4)
        passed = fixed + (places - fixed + offset_by * (used - fixed)) % max(1, number_of - fixed)
        return jnp.zeros((number_of,), jnp.int32).at[sequence[jnp.where(places < fixed, places, passed)]].set(jnp.asarray(tallies, jnp.int32))

    tallies = jnp.where(number % 4 == 0, named(heavy_load, number // 4), named(ordinary, number - number // 4 - 1))
    mixed = jax.random.permutation(jax.random.fold_in(own, 3), number_of)
    giver, sink = mixed[0:number_of // 2 * 2:2], mixed[1:number_of // 2 * 2:2]
    margin = jnp.minimum(tallies[giver] - 1, bound - tallies[sink]) // 2
    margin = jnp.where((giver == sequence[0]) | (sink == sequence[0]) | (tallies[sink] == 0), 0, jnp.maximum(margin, 0))
    passed = jax.random.randint(jax.random.fold_in(own, 4), (number_of // 2,), 0, 1 << 20) % (margin + 1)
    tallies = tallies.at[giver].add(-passed).at[sink].add(passed)
    members = jnp.searchsorted(jnp.cumsum(tallies), jnp.arange(rows * top), side="right").astype(jnp.int32)
    listing = members.reshape(top, rows).T
    listing = listing[jax.random.permutation(jax.random.fold_in(own, 1), rows)]
    offset_by = jax.random.randint(jax.random.fold_in(own, 2), (rows, 1), 0, top)
    return jnp.take_along_axis(listing, (jnp.arange(top)[None, :] + offset_by) % top, axis=1)


def shares(count, total, most, skew, full):
    portions = [(1 << 20) // math.isqrt(grade ** skew) + 1 for grade in range(1, count + 1)]
    largest = most if full else min(most, max(-(-total // count), total * portions[0] // sum(portions)))
    least = 1 if total - largest >= count - 1 else 0
    given, rest = [largest] + [least] * (count - 1), total - largest - least * (count - 1)
    while rest > 0:
        candidates = [i for i in range(1, count) if given[i] < largest] or [i for i in range(1, count) if given[i] < most]
        whole, budget = sum([portions[i] for i in candidates]), rest
        for i in candidates:
            extra = min(most - given[i], max(1, budget * portions[i] // whole), rest)
            given[i] = given[i] + extra
            rest = rest - extra
    return np.array(given)


def normal_values(own_key, dims, spread, limit, pieces=(), kind=jnp.bfloat16):
    values = spread * jax.random.normal(own_key, dims, jnp.float32)
    if pieces:
        values = values * block_levels(own_key, dims, pieces, -0.22, 0.18)
    return jnp.clip(values, -limit, limit).astype(kind)


def setup_inputs(seed: int = 0) -> dict:
    arg_keys = jax.random.split(jax.random.key(seed), 22)
    tokens = normal_values(arg_keys[0], (TOKENS, D), 1.0, 6.0, ((0, 32),))
    gain_mix = jnp.clip(1.0 + 0.18 * jax.random.normal(arg_keys[1], (D,), jnp.float32), 0.1, 1.9)
    w_query = normal_values(arg_keys[2], (D, HEADS * DK), D ** -0.5, 0.125)
    w_key = normal_values(arg_keys[3], (D, HEADS * DK), D ** -0.5, 0.125)
    w_value = normal_values(arg_keys[4], (D, HEADS * DV), D ** -0.5, 0.125)
    w_input_gate = normal_values(arg_keys[5], (D, HEADS), D ** -0.5, 0.125)
    w_forget_gate = normal_values(arg_keys[6], (D, HEADS), D ** -0.5, 0.125)
    bias_input = jnp.clip(jax.random.uniform(arg_keys[7], (HEADS,), jnp.float32, -1.0, 1.0), -1.0, 1.0)
    bias_forget = jnp.clip(jax.random.uniform(arg_keys[8], (HEADS,), jnp.float32, 0.0, 5.0), 0.0, 5.0)
    memory_cells = normal_values(arg_keys[9], (TOKENS, HEADS, DK, DV), 1.0, 6.0, ((0, 32),), jnp.float32)
    normalizer = normal_values(arg_keys[10], (TOKENS, HEADS, DK), 1.0, 6.0, ((0, 32),), jnp.float32)
    stabilizer = jnp.clip(jax.random.uniform(arg_keys[11], (TOKENS, HEADS), jnp.float32, -1.0, 1.0) * block_levels(arg_keys[11], (TOKENS, HEADS), ((0, 32),), -0.4, 0.0), -1.0, 1.0)
    w_mix_out = normal_values(arg_keys[12], (HEADS * DV, D), (HEADS * DV) ** -0.5, 0.21875)
    gain_mix_post = jnp.clip(1.0 + 0.18 * jax.random.normal(arg_keys[13], (D,), jnp.float32), 0.1, 1.9)
    gain_ffn = jnp.clip(1.0 + 0.18 * jax.random.normal(arg_keys[14], (D,), jnp.float32), 0.1, 1.9)
    w_router = normal_values(arg_keys[15], (D, EXPERTS), D ** -0.5, 0.125)
    routing_keys = jax.random.split(jax.random.fold_in(arg_keys[16], 1), TOKENS // SEQ_DEV)
    routing_turns = jax.random.permutation(jax.random.fold_in(arg_keys[16], 3), TOKENS // SEQ_DEV)
    routing = jax.vmap(lambda own, number: routed_block(jax.random.fold_in(arg_keys[16], 2), own, number, SEQ_DEV, EXPERTS, TOP_K, CAP, 2))(routing_keys, routing_turns).reshape((TOKENS, TOP_K))
    w_expert_gate = normal_values(arg_keys[17], (EXPERTS * SPLIT, D, FF_E // SPLIT), D ** -0.5, 0.125, ((0, 32),))
    w_expert_up = normal_values(arg_keys[18], (EXPERTS * SPLIT, D, FF_E // SPLIT), D ** -0.5, 0.125, ((0, 32),))
    w_expert_down = normal_values(arg_keys[19], (EXPERTS * SPLIT, FF_E // SPLIT, D), FF_E ** -0.5, 0.15625, ((0, 32),))
    gain_ffn_post = jnp.clip(1.0 + 0.18 * jax.random.normal(arg_keys[20], (D,), jnp.float32), 0.1, 1.9)
    return dict(tokens=tokens, gain_mix=gain_mix, w_query=w_query, w_key=w_key, w_value=w_value, w_input_gate=w_input_gate, w_forget_gate=w_forget_gate, bias_input=bias_input, bias_forget=bias_forget, memory_cells=memory_cells, normalizer=normalizer, stabilizer=stabilizer, w_mix_out=w_mix_out, gain_mix_post=gain_mix_post, gain_ffn=gain_ffn, w_router=w_router, routing=routing, w_expert_gate=w_expert_gate, w_expert_up=w_expert_up, w_expert_down=w_expert_down, gain_ffn_post=gain_ffn_post)


epsilon = 1e-06

def normalize(values, gain):
    return values * lax.rsqrt(lax.optimization_barrier(jnp.mean(values * values, axis=-1, keepdims=True)) + epsilon) * gain

def rounded(values):
    return lax.optimization_barrier(values.astype(jnp.bfloat16)).astype(jnp.float32)

def cell_step(normed, w_query, w_key, w_value, w_input_gate, w_forget_gate, bias_input, bias_forget, memory_cells, normalizer, stabilizer):
    row_count, heads, key_size, value_size = memory_cells.shape
    query_rows = rounded(jnp.dot(normed, w_query, preferred_element_type=jnp.float32))
    query_rows = query_rows.reshape(row_count, heads, key_size) * key_size ** (-0.5)
    key_rows = rounded(jnp.dot(normed, w_key, preferred_element_type=jnp.float32)).reshape(row_count, heads, key_size)
    value_rows = rounded(jnp.dot(normed, w_value, preferred_element_type=jnp.float32)).reshape(row_count, heads, value_size)
    input_gate = jnp.dot(normed, w_input_gate, preferred_element_type=jnp.float32) + bias_input
    log_forget = jax.nn.log_sigmoid(jnp.dot(normed, w_forget_gate, preferred_element_type=jnp.float32) + bias_forget)
    carried = log_forget + stabilizer
    stab_next = jnp.maximum(carried, input_gate)
    keep_weight = jnp.exp(carried - stab_next)
    write_weight = jnp.exp(input_gate - stab_next)
    scaled_keys = write_weight[:, :, None] * key_rows
    cells_next = keep_weight[:, :, None, None] * memory_cells + scaled_keys[:, :, :, None] * value_rows[:, :, None, :]
    norm_next = keep_weight[:, :, None] * normalizer + scaled_keys
    numerator = jnp.einsum('bhd,bhde->bhe', query_rows, cells_next, precision=lax.Precision.HIGHEST)
    denominator = jnp.einsum('bhd,bhd->bh', query_rows, norm_next, precision=lax.Precision.HIGHEST)
    denominator = jnp.maximum(jnp.abs(denominator), jnp.exp(-stab_next))
    cell_out = (numerator / denominator[:, :, None]).reshape(row_count, heads * value_size).astype(jnp.bfloat16)
    return (cell_out, cells_next, norm_next, stab_next)

def route_weights(rows_in, w_router, routes):
    logits = jnp.dot(rows_in, w_router, preferred_element_type=jnp.float32)
    onehot = routes[:, :, None] == jnp.arange(w_router.shape[1], dtype=jnp.int32)[None, None, :]
    chosen = lax.optimization_barrier(jnp.sum(jnp.where(onehot, logits[:, None, :], 0.0), axis=-1))
    return jax.nn.sigmoid(chosen - chosen[:, ::-1])

def expert_partial(row_block, gate_w, up_w, down_w):
    gate_part = jnp.dot(row_block, gate_w, preferred_element_type=jnp.float32)
    up_part = jnp.dot(row_block, up_w, preferred_element_type=jnp.float32)
    hidden = (jax.nn.silu(gate_part) * up_part).astype(jnp.bfloat16)
    return rounded(jnp.dot(hidden, down_w, preferred_element_type=jnp.float32))

def reference(tokens, gain_mix, w_query, w_key, w_value, w_input_gate, w_forget_gate, bias_input, bias_forget, memory_cells, normalizer, stabilizer, w_mix_out, gain_mix_post, gain_ffn, w_router, routing, w_expert_gate, w_expert_up, w_expert_down, gain_ffn_post):
    residual = tokens.astype(jnp.float32)
    normed = normalize(residual, gain_mix).astype(jnp.bfloat16)
    cell_out, cells_next, norm_next, stab_next = cell_step(normed, w_query, w_key, w_value, w_input_gate, w_forget_gate, bias_input, bias_forget, memory_cells, normalizer, stabilizer)
    mix_out = jnp.dot(cell_out, w_mix_out, preferred_element_type=jnp.float32)
    after_mix = (residual + normalize(mix_out, gain_mix_post)).astype(jnp.bfloat16)
    after_float = after_mix.astype(jnp.float32)
    expert_in = normalize(after_float, gain_ffn).astype(jnp.bfloat16)
    route_weight = route_weights(expert_in, w_router, routing)
    onehot = (routing[:, :, None] == jnp.arange(EXPERTS, dtype=jnp.int32)[None, None, :]).astype(jnp.int32)
    flat_hot = onehot.reshape(N_EP, SEQ_DEV * TOP_K, EXPERTS)
    slot_index = lax.optimization_barrier(jnp.sum((jnp.cumsum(flat_hot, axis=1) - 1) * flat_hot, axis=-1))
    position = (jnp.arange(N_EP, dtype=jnp.int32)[:, None] * CAP + slot_index).reshape(-1).astype(jnp.int32)
    expert_index = routing.reshape(-1).astype(jnp.int32)
    repeated = jnp.repeat(expert_in, TOP_K, axis=0)
    buffer = jnp.zeros((EXPERTS, N_EP * CAP, D), jnp.bfloat16).at[expert_index, position].set(repeated)
    quarter_width = FF_E // SPLIT
    gate_all = w_expert_gate.reshape(EXPERTS, SPLIT, D, quarter_width)
    up_all = w_expert_up.reshape(EXPERTS, SPLIT, D, quarter_width)
    down_all = w_expert_down.reshape(EXPERTS, SPLIT, quarter_width, D)

    def serve(operands):
        row_block, gate_w, up_w, down_w = operands
        running = jnp.zeros((row_block.shape[0], D), jnp.float32)
        for quarter_index in range(SPLIT):
            running = running + expert_partial(row_block, gate_w[quarter_index], up_w[quarter_index], down_w[quarter_index])
        return running
    results = lax.map(serve, (buffer, gate_all, up_all, down_all))
    picked = results[expert_index, position]
    expert_sum = lax.optimization_barrier(jnp.sum((picked * route_weight.reshape(-1, 1)).reshape(-1, TOP_K, D), axis=1))
    mixed = (after_float + normalize(expert_sum, gain_ffn_post)).astype(jnp.bfloat16)
    return (mixed, cells_next, norm_next, stab_next)
```

```python
import functools

import jax
import jax.numpy as jnp
from jax import lax
from jax.experimental import pallas as pl
from jax.experimental.pallas import tpu as pltpu
from jax.sharding import PartitionSpec as P

epsilon = 1e-06


def normalize(values, gain):
    return values * lax.rsqrt(jnp.mean(values * values, axis=-1, keepdims=True) + epsilon) * gain


def rounded(values):
    return lax.optimization_barrier(values.astype(jnp.bfloat16)).astype(jnp.float32)


def cell_step(
    normed,
    w_query,
    w_key,
    w_value,
    w_input_gate,
    w_forget_gate,
    bias_input,
    bias_forget,
    memory_cells,
    normalizer,
    stabilizer,
):
    row_count, heads, key_size, value_size = memory_cells.shape
    query_rows = rounded(jnp.dot(normed, w_query, preferred_element_type=jnp.float32))
    query_rows = query_rows.reshape(row_count, heads, key_size) * key_size ** (-0.5)
    key_rows = rounded(jnp.dot(normed, w_key, preferred_element_type=jnp.float32)).reshape(
        row_count, heads, key_size
    )
    value_rows = rounded(jnp.dot(normed, w_value, preferred_element_type=jnp.float32)).reshape(
        row_count, heads, value_size
    )
    input_gate = jnp.dot(normed, w_input_gate, preferred_element_type=jnp.float32) + bias_input
    log_forget = jax.nn.log_sigmoid(
        jnp.dot(normed, w_forget_gate, preferred_element_type=jnp.float32) + bias_forget
    )
    carried = log_forget + stabilizer
    stab_next = jnp.maximum(carried, input_gate)
    keep_weight = jnp.exp(carried - stab_next)
    write_weight = jnp.exp(input_gate - stab_next)
    scaled_keys = write_weight[:, :, None] * key_rows
    cells_next = (
        keep_weight[:, :, None, None] * memory_cells
        + scaled_keys[:, :, :, None] * value_rows[:, :, None, :]
    )
    norm_next = keep_weight[:, :, None] * normalizer + scaled_keys
    numerator = jnp.einsum("bhd,bhde->bhe", query_rows, cells_next, precision=lax.Precision.HIGHEST)
    denominator = jnp.einsum("bhd,bhd->bh", query_rows, norm_next, precision=lax.Precision.HIGHEST)
    denominator = jnp.maximum(jnp.abs(denominator), jnp.exp(-stab_next))
    cell_out = (
        (numerator / denominator[:, :, None])
        .reshape(row_count, heads * value_size)
        .astype(jnp.bfloat16)
    )
    return (cell_out, cells_next, norm_next, stab_next)


def route_weights(rows_in, w_router, routes):
    logits = jnp.dot(rows_in, w_router, preferred_element_type=jnp.float32)
    onehot = routes[:, :, None] == jnp.arange(w_router.shape[1], dtype=jnp.int32)[None, None, :]
    chosen = jnp.sum(jnp.where(onehot, logits[:, None, :], 0.0), axis=-1)
    return jax.nn.sigmoid(chosen - chosen[:, ::-1])


def expert_quarter(row_block, gate_w, up_w, down_w):
    gate_part = jnp.dot(row_block, gate_w, preferred_element_type=jnp.float32)
    up_part = jnp.dot(row_block, up_w, preferred_element_type=jnp.float32)
    hidden = (jax.nn.silu(gate_part) * up_part).astype(jnp.bfloat16)
    return jnp.dot(hidden, down_w, preferred_element_type=jnp.float32).astype(jnp.bfloat16)


VMEM = pl.BlockSpec(memory_space=pltpu.VMEM)


def remote_copy(src, dst, sems, kind, step, target):
    return pltpu.make_async_remote_copy(
        src_ref=src,
        dst_ref=dst,
        send_sem=sems[0].at[kind, step],
        recv_sem=sems[1].at[kind, step],
        device_id=(target,),
        device_id_type=pl.DeviceIdType.MESH,
    )


def places(group_size):
    me = lax.axis_index("ep")
    own = lax.div(me, group_size)
    member = lax.rem(me, group_size)
    core_mate = member + 1 - 2 * lax.rem(member, 2)
    chip_mate = lax.rem(member + 2, group_size)
    far_mate = lax.rem(core_mate + 2, group_size)
    return own, member, core_mate, chip_mate, far_mate


def greet(experts, group_size):
    own, member, core_mate, chip_mate, _ = places(group_size)
    barrier = pltpu.get_barrier_semaphore()

    def signal(target):
        pl.semaphore_signal(
            barrier, inc=1, device_id=(target,), device_id_type=pl.DeviceIdType.MESH
        )

    for step in range(1, experts):
        signal(lax.rem(own + step, experts) * group_size + member)
    signal(own * group_size + core_mate)
    signal(own * group_size + chip_mate)
    pl.semaphore_wait(barrier, experts + 1)


def dispatch_kernel(experts, group_size, outgoing, arrived, send_sems, recv_sems):
    own, member, core_mate, chip_mate, _ = places(group_size)
    sems = (send_sems, recv_sems)
    greet(experts, group_size)

    def direct(step):
        target = lax.rem(own + step, experts)
        return remote_copy(
            outgoing.at[target],
            arrived.at[own, member],
            sems,
            0,
            step,
            target * group_size + member,
        )

    def forward(step, kind):
        source = lax.rem(own + experts - step, experts)
        mate = core_mate if kind != 2 else chip_mate
        row = member if kind != 3 else chip_mate
        src = arrived.at[source, row]
        if step == 0 and kind != 3:
            src = outgoing.at[own]
        return remote_copy(
            src, arrived.at[source, row], sems, kind, step, own * group_size + mate
        )

    for step in range(1, experts):
        direct(step).start()
    forward(0, 2).start()
    forward(0, 1).start()
    arrived[own, member] = outgoing[own]
    for step in range(1, experts):
        direct(step).wait_recv()
        forward(step, 2).start()
        forward(step, 1).start()
        forward(step - 1, 2).wait_recv()
        forward(step - 1, 3).start()
    forward(experts - 1, 2).wait_recv()
    forward(experts - 1, 3).start()
    for step in range(experts):
        if step:
            direct(step).wait_send()
        forward(step, 2).wait_send()
        forward(step, 1).wait()
        forward(step, 3).wait()


def dispatch_rows(outgoing, group_size):
    experts, capacity, width = outgoing.shape
    return pl.pallas_call(
        functools.partial(dispatch_kernel, experts, group_size),
        out_shape=jax.ShapeDtypeStruct((experts, group_size, capacity, width), outgoing.dtype),
        in_specs=[VMEM],
        out_specs=VMEM,
        scratch_shapes=[
            pltpu.SemaphoreType.DMA((4, experts)),
            pltpu.SemaphoreType.DMA((4, experts)),
        ],
        compiler_params=pltpu.CompilerParams(collective_id=0, has_side_effects=True),
        name="dispatch_rows",
    )(outgoing)


def return_kernel(
    experts,
    group_size,
    computed,
    returned,
    core_in,
    chip_out,
    chip_in,
    final_out,
    send_sems,
    recv_sems,
):
    own, member, core_mate, chip_mate, far_mate = places(group_size)
    sems = (send_sems, recv_sems)
    greet(experts, group_size)

    def source_of(step):
        return lax.rem(own + step, experts)

    def to_core(step, kind):
        row = core_mate if kind == 0 else far_mate
        return remote_copy(
            computed.at[source_of(step), row],
            core_in.at[kind, step],
            sems,
            kind,
            step,
            own * group_size + core_mate,
        )

    def to_chip(step):
        return remote_copy(
            chip_out.at[step], chip_in.at[step], sems, 2, step, own * group_size + chip_mate
        )

    def to_source(step):
        target = source_of(step)
        return remote_copy(
            final_out.at[step], returned.at[own], sems, 3, step, target * group_size + member
        )

    def wide(values):
        return values.astype(jnp.float32)

    order = list(range(1, experts)) + [0]
    for step in order:
        to_core(step, 1).start()
        to_core(step, 0).start()
    before = None
    for step in order:
        to_core(step, 1).wait_recv()
        total = wide(computed[source_of(step), chip_mate]) + wide(core_in[1, step])
        chip_out[step] = total.astype(chip_out.dtype)
        if before is not None:
            to_chip(before).start()
        before = step
    for step in order:
        to_core(step, 0).wait_recv()
        if before is not None:
            to_chip(before).start()
            before = None
    for step in order:
        to_chip(step).wait_recv()
        total = wide(computed[source_of(step), member]) + wide(core_in[0, step])
        total = (total + wide(chip_in[step])).astype(final_out.dtype)
        if step:
            final_out[step] = total
        else:
            returned[own] = total
        if before is not None:
            to_source(before).start()
        before = step if step else None
    for step in range(experts):
        to_core(step, 0).wait_send()
        to_core(step, 1).wait_send()
        to_chip(step).wait_send()
        if step:
            to_source(step).wait()


def return_rows(computed):
    experts, group_size, capacity, width = computed.shape
    chunk = (experts, capacity, width)
    return pl.pallas_call(
        functools.partial(return_kernel, experts, group_size),
        out_shape=jax.ShapeDtypeStruct(chunk, computed.dtype),
        in_specs=[VMEM],
        out_specs=VMEM,
        scratch_shapes=[
            pltpu.VMEM((2,) + chunk, computed.dtype),
            pltpu.VMEM(chunk, computed.dtype),
            pltpu.VMEM(chunk, computed.dtype),
            pltpu.VMEM(chunk, computed.dtype),
            pltpu.SemaphoreType.DMA((4, experts)),
            pltpu.SemaphoreType.DMA((4, experts)),
        ],
        compiler_params=pltpu.CompilerParams(collective_id=1, has_side_effects=True),
        name="return_rows",
    )(computed)


def body(
    tokens,
    gain_mix,
    w_query,
    w_key,
    w_value,
    w_input_gate,
    w_forget_gate,
    bias_input,
    bias_forget,
    memory_cells,
    normalizer,
    stabilizer,
    w_mix_out,
    gain_mix_post,
    gain_ffn,
    w_router,
    routing,
    w_expert_gate,
    w_expert_up,
    w_expert_down,
    gain_ffn_post,
):
    devices = lax.axis_size("ep")
    device_index = lax.axis_index("ep")
    seq_rows = tokens.shape[0]
    model_width = tokens.shape[1]
    experts = w_router.shape[1]
    group_size = devices // experts
    top_count = routing.shape[1]
    capacity = max(2, seq_rows * top_count * 2 // experts)
    residual = tokens.astype(jnp.float32)
    normed = normalize(residual, gain_mix).astype(jnp.bfloat16)
    cell_out, cells_next, norm_next, stab_next = cell_step(
        normed,
        w_query,
        w_key,
        w_value,
        w_input_gate,
        w_forget_gate,
        bias_input,
        bias_forget,
        memory_cells,
        normalizer,
        stabilizer,
    )
    mix_out = jnp.dot(cell_out, w_mix_out, preferred_element_type=jnp.float32)
    after_mix = (residual + normalize(mix_out, gain_mix_post)).astype(jnp.bfloat16)
    after_float = after_mix.astype(jnp.float32)
    expert_in = normalize(after_float, gain_ffn).astype(jnp.bfloat16)
    gate_w = w_expert_gate[0]
    up_w = w_expert_up[0]
    down_w = w_expert_down[0]
    own_routes = lax.dynamic_slice_in_dim(routing, device_index * seq_rows, seq_rows, 0)
    route_weight = route_weights(expert_in, w_router, own_routes)
    flat_routes = own_routes.reshape(-1)
    flat_hot = (flat_routes[:, None] == jnp.arange(experts, dtype=jnp.int32)[None, :]).astype(
        jnp.int32
    )
    slot_index = jnp.sum((jnp.cumsum(flat_hot, axis=0) - 1) * flat_hot, axis=1)
    position = (flat_routes * capacity + slot_index).reshape(seq_rows, top_count)
    placed = position[:, :, None] == jnp.arange(experts * capacity, dtype=jnp.int32)
    dispatch = jnp.any(placed, axis=1).astype(jnp.bfloat16)
    outgoing = jnp.einsum(
        "rp,rd->pd", dispatch, expert_in, preferred_element_type=jnp.float32
    ).astype(jnp.bfloat16)
    arrived = dispatch_rows(outgoing.reshape(experts, capacity, model_width), group_size)
    computed = expert_quarter(arrived.reshape(-1, model_width), gate_w, up_w, down_w)
    returned = return_rows(computed.reshape(arrived.shape))
    summed = returned.astype(jnp.float32).reshape(experts * capacity, model_width)
    combine = jnp.sum(jnp.where(placed, route_weight[:, :, None], 0.0), axis=1)
    expert_sum = jnp.dot(combine, summed, precision=lax.Precision.HIGHEST)
    mixed = (after_float + normalize(expert_sum, gain_ffn_post)).astype(jnp.bfloat16)
    return (mixed, cells_next, norm_next, stab_next)


def solution(mesh):
    return jax.shard_map(
        body,
        mesh=mesh,
        in_specs=(
            P("ep", None),
            P(),
            P(),
            P(),
            P(),
            P(),
            P(),
            P(),
            P(),
            P("ep", None, None, None),
            P("ep", None, None),
            P("ep", None),
            P(),
            P(),
            P(),
            P(),
            P(),
            P("ep", None, None),
            P("ep", None, None),
            P("ep", None, None),
            P(),
        ),
        out_specs=(P("ep", None), P("ep", None, None, None), P("ep", None, None), P("ep", None)),
        check_vma=False,
    )
```

```python
import functools

import jax
import jax.numpy as jnp
from jax import lax
from jax.experimental import pallas as pl
from jax.experimental.pallas import tpu as pltpu
from jax.sharding import PartitionSpec as P

epsilon = 1e-06


def normalize(values, gain):
    return values * lax.rsqrt(jnp.mean(values * values, axis=-1, keepdims=True) + epsilon) * gain


def rounded(values):
    return lax.optimization_barrier(values.astype(jnp.bfloat16)).astype(jnp.float32)


def cell_kernel(keep, cells, queries, keys, values, cells_next, numerator):
    block, heads, key_size, value_size = cells.shape
    first = pl.program_id(0) * block
    for row in range(block):
        for head in range(heads):
            span = slice(head * key_size, (head + 1) * key_size)
            key_column = keys[0, span, row : row + 1]
            query_column = queries[0, span, row : row + 1]
            value_row = values[row, head : head + 1, :]
            updated = keep[first + row, head] * cells[row, head] + key_column * value_row
            cells_next[row, head] = updated
            numerator[row, head : head + 1, :] = jnp.sum(
                query_column * updated, axis=0, keepdims=True
            )


def update_cells(keep, cells, queries, keys, values):
    rows, heads, key_size, value_size = cells.shape
    block = next(size for size in (4, 2, 1) if rows % size == 0)

    def columns(array):
        flat = array.reshape(rows // block, block, heads * key_size)
        return jnp.swapaxes(flat, 1, 2)

    cell_spec = pl.BlockSpec((block, heads, key_size, value_size), lambda i: (i, 0, 0, 0))
    column_spec = pl.BlockSpec((1, heads * key_size, block), lambda i: (i, 0, 0))
    value_spec = pl.BlockSpec((block, heads, value_size), lambda i: (i, 0, 0))
    return pl.pallas_call(
        cell_kernel,
        grid=(rows // block,),
        out_shape=(
            jax.ShapeDtypeStruct(cells.shape, jnp.float32),
            jax.ShapeDtypeStruct(values.shape, jnp.float32),
        ),
        in_specs=[
            pl.BlockSpec(memory_space=pltpu.SMEM),
            cell_spec,
            column_spec,
            column_spec,
            value_spec,
        ],
        out_specs=(cell_spec, value_spec),
        compiler_params=pltpu.CompilerParams(vmem_limit_bytes=16 * 2**20),
        name="update_cells",
    )(keep, cells, columns(queries), columns(keys), values)


def cell_step(
    normed,
    w_query,
    w_key,
    w_value,
    w_input_gate,
    w_forget_gate,
    bias_input,
    bias_forget,
    memory_cells,
    normalizer,
    stabilizer,
):
    row_count, heads, key_size, value_size = memory_cells.shape
    query_rows = rounded(jnp.dot(normed, w_query, preferred_element_type=jnp.float32))
    query_rows = query_rows.reshape(row_count, heads, key_size) * key_size ** (-0.5)
    key_rows = rounded(jnp.dot(normed, w_key, preferred_element_type=jnp.float32)).reshape(
        row_count, heads, key_size
    )
    value_rows = rounded(jnp.dot(normed, w_value, preferred_element_type=jnp.float32)).reshape(
        row_count, heads, value_size
    )
    input_gate = jnp.dot(normed, w_input_gate, preferred_element_type=jnp.float32) + bias_input
    log_forget = jax.nn.log_sigmoid(
        jnp.dot(normed, w_forget_gate, preferred_element_type=jnp.float32) + bias_forget
    )
    carried = log_forget + stabilizer
    stab_next = jnp.maximum(carried, input_gate)
    keep_weight = jnp.exp(carried - stab_next)
    write_weight = jnp.exp(input_gate - stab_next)
    scaled_keys = write_weight[:, :, None] * key_rows
    norm_next = keep_weight[:, :, None] * normalizer + scaled_keys
    cells_next, numerator = update_cells(
        keep_weight, memory_cells, query_rows, scaled_keys, value_rows
    )
    denominator = jnp.einsum("bhd,bhd->bh", query_rows, norm_next, precision=lax.Precision.HIGHEST)
    denominator = jnp.maximum(jnp.abs(denominator), jnp.exp(-stab_next))
    cell_out = (
        (numerator / denominator[:, :, None])
        .reshape(row_count, heads * value_size)
        .astype(jnp.bfloat16)
    )
    return (cell_out, cells_next, norm_next, stab_next)


def route_weights(rows_in, w_router, routes):
    logits = jnp.dot(rows_in, w_router, preferred_element_type=jnp.float32)
    onehot = routes[:, :, None] == jnp.arange(w_router.shape[1], dtype=jnp.int32)[None, None, :]
    chosen = jnp.sum(jnp.where(onehot, logits[:, None, :], 0.0), axis=-1)
    return jax.nn.sigmoid(chosen - chosen[:, ::-1])


VMEM = pl.BlockSpec(memory_space=pltpu.VMEM)


def remote_copy(src, dst, sems, kind, step, target):
    return pltpu.make_async_remote_copy(
        src_ref=src,
        dst_ref=dst,
        send_sem=sems[0].at[kind, step],
        recv_sem=sems[1].at[kind, step],
        device_id=(target,),
        device_id_type=pl.DeviceIdType.MESH,
    )


def places(group_size):
    me = lax.axis_index("ep")
    own = lax.div(me, group_size)
    member = lax.rem(me, group_size)
    core_mate = member + 1 - 2 * lax.rem(member, 2)
    chip_mate = lax.rem(member + 2, group_size)
    far_mate = lax.rem(core_mate + 2, group_size)
    return own, member, core_mate, chip_mate, far_mate


def paired(own, step):
    other = own
    bit = 1
    while bit <= step:
        if step & bit:
            other = other + bit - 2 * bit * lax.rem(lax.div(own, bit), 2)
        bit *= 2
    return other


def greet(experts, group_size):
    own, member, core_mate, chip_mate, _ = places(group_size)
    barrier = pltpu.get_barrier_semaphore()

    def signal(target):
        pl.semaphore_signal(
            barrier, inc=1, device_id=(target,), device_id_type=pl.DeviceIdType.MESH
        )

    for step in range(1, experts):
        signal(paired(own, step) * group_size + member)
    signal(own * group_size + core_mate)
    signal(own * group_size + chip_mate)
    pl.semaphore_wait(barrier, experts + 1)


def dispatch_kernel(experts, group_size, outgoing, arrived, send_sems, recv_sems):
    own, member, core_mate, chip_mate, _ = places(group_size)
    sems = (send_sems, recv_sems)
    greet(experts, group_size)

    def direct(step):
        target = paired(own, step)
        return remote_copy(
            outgoing.at[target],
            arrived.at[own, member],
            sems,
            0,
            step,
            target * group_size + member,
        )

    def forward(step, kind):
        source = paired(own, step)
        mate = core_mate if kind != 2 else chip_mate
        row = member if kind != 3 else chip_mate
        src = arrived.at[source, row]
        if step == 0 and kind != 3:
            src = outgoing.at[own]
        return remote_copy(
            src, arrived.at[source, row], sems, kind, step, own * group_size + mate
        )

    for step in range(1, experts):
        direct(step).start()
    forward(0, 2).start()
    forward(0, 1).start()
    arrived[own, member] = outgoing[own]
    for step in range(1, experts):
        direct(step).wait_recv()
        forward(step, 2).start()
        forward(step, 1).start()
        forward(step - 1, 2).wait_recv()
        forward(step - 1, 3).start()
    forward(experts - 1, 2).wait_recv()
    forward(experts - 1, 3).start()
    for step in range(experts):
        if step:
            direct(step).wait_send()
        forward(step, 2).wait_send()
        forward(step, 1).wait()
        forward(step, 3).wait()


def expert_kernel(rows_in, gate_w, up_w, down_w, result):
    rows = rows_in.shape[0]
    pieces = 2 if rows % 512 == 0 else 1
    for piece in range(pieces):
        span = slice(piece * rows // pieces, (piece + 1) * rows // pieces)
        block = rows_in[span, :]
        gate_part = jnp.dot(block, gate_w[0], preferred_element_type=jnp.float32)
        up_part = jnp.dot(block, up_w[0], preferred_element_type=jnp.float32)
        hidden = (jax.nn.silu(gate_part) * up_part).astype(rows_in.dtype)
        result[span, :] = jnp.dot(
            hidden, down_w[0], preferred_element_type=jnp.float32
        ).astype(result.dtype)


def expert_quarter(rows_in, gate_w, up_w, down_w):
    return pl.pallas_call(
        expert_kernel,
        out_shape=jax.ShapeDtypeStruct(rows_in.shape, rows_in.dtype),
        in_specs=[VMEM] * 4,
        out_specs=VMEM,
        compiler_params=pltpu.CompilerParams(vmem_limit_bytes=24 * 2**20),
        name="expert_quarter",
    )(rows_in, gate_w, up_w, down_w)


def dispatch_rows(outgoing, group_size):
    experts, capacity, width = outgoing.shape
    return pl.pallas_call(
        functools.partial(dispatch_kernel, experts, group_size),
        out_shape=jax.ShapeDtypeStruct((experts, group_size, capacity, width), outgoing.dtype),
        in_specs=[VMEM],
        out_specs=VMEM,
        scratch_shapes=[
            pltpu.SemaphoreType.DMA((4, experts)),
            pltpu.SemaphoreType.DMA((4, experts)),
        ],
        compiler_params=pltpu.CompilerParams(
            collective_id=0, has_side_effects=True, vmem_limit_bytes=12 * 2**20
        ),
        name="dispatch_rows",
    )(outgoing)


def return_kernel(
    experts,
    group_size,
    computed,
    returned,
    core_in,
    chip_out,
    chip_in,
    final_out,
    send_sems,
    recv_sems,
):
    own, member, core_mate, chip_mate, far_mate = places(group_size)
    sems = (send_sems, recv_sems)
    greet(experts, group_size)

    def source_of(step):
        return paired(own, step)

    def to_core(step, kind):
        row = core_mate if kind == 0 else far_mate
        return remote_copy(
            computed.at[source_of(step), row],
            core_in.at[kind, step],
            sems,
            kind,
            step,
            own * group_size + core_mate,
        )

    def to_chip(step):
        return remote_copy(
            chip_out.at[step], chip_in.at[step], sems, 2, step, own * group_size + chip_mate
        )

    def to_source(step):
        target = source_of(step)
        return remote_copy(
            final_out.at[step], returned.at[own], sems, 3, step, target * group_size + member
        )

    def wide(values):
        return values.astype(jnp.float32)

    order = list(range(experts - 1, -1, -1))
    for step in order:
        to_core(step, 1).start()
        to_core(step, 0).start()
    before = None
    for step in order:
        to_core(step, 1).wait_recv()
        total = wide(computed[source_of(step), chip_mate]) + wide(core_in[1, step])
        chip_out[step] = total.astype(chip_out.dtype)
        if before is not None:
            to_chip(before).start()
        before = step
    for step in order:
        to_core(step, 0).wait_recv()
        if before is not None:
            to_chip(before).start()
            before = None
    for step in order:
        to_chip(step).wait_recv()
        total = wide(computed[source_of(step), member]) + wide(core_in[0, step])
        total = (total + wide(chip_in[step])).astype(final_out.dtype)
        if step:
            final_out[step] = total
        else:
            returned[own] = total
        if before is not None:
            to_source(before).start()
        before = step if step else None
    for step in range(experts):
        to_core(step, 0).wait_send()
        to_core(step, 1).wait_send()
        to_chip(step).wait_send()
        if step:
            to_source(step).wait()


def return_rows(computed):
    experts, group_size, capacity, width = computed.shape
    chunk = (experts, capacity, width)
    return pl.pallas_call(
        functools.partial(return_kernel, experts, group_size),
        out_shape=jax.ShapeDtypeStruct(chunk, computed.dtype),
        in_specs=[VMEM],
        out_specs=VMEM,
        scratch_shapes=[
            pltpu.VMEM((2,) + chunk, computed.dtype),
            pltpu.VMEM(chunk, computed.dtype),
            pltpu.VMEM(chunk, computed.dtype),
            pltpu.VMEM(chunk, computed.dtype),
            pltpu.SemaphoreType.DMA((4, experts)),
            pltpu.SemaphoreType.DMA((4, experts)),
        ],
        compiler_params=pltpu.CompilerParams(
            collective_id=1, has_side_effects=True, vmem_limit_bytes=16 * 2**20
        ),
        name="return_rows",
    )(computed)


def body(
    tokens,
    gain_mix,
    w_query,
    w_key,
    w_value,
    w_input_gate,
    w_forget_gate,
    bias_input,
    bias_forget,
    memory_cells,
    normalizer,
    stabilizer,
    w_mix_out,
    gain_mix_post,
    gain_ffn,
    w_router,
    routing,
    w_expert_gate,
    w_expert_up,
    w_expert_down,
    gain_ffn_post,
):
    devices = lax.axis_size("ep")
    device_index = lax.axis_index("ep")
    seq_rows = tokens.shape[0]
    model_width = tokens.shape[1]
    experts = w_router.shape[1]
    group_size = devices // experts
    top_count = routing.shape[1]
    capacity = max(2, seq_rows * top_count * 2 // experts)
    residual = tokens.astype(jnp.float32)
    normed = normalize(residual, gain_mix).astype(jnp.bfloat16)
    cell_out, cells_next, norm_next, stab_next = cell_step(
        normed,
        w_query,
        w_key,
        w_value,
        w_input_gate,
        w_forget_gate,
        bias_input,
        bias_forget,
        memory_cells,
        normalizer,
        stabilizer,
    )
    mix_out = jnp.dot(cell_out, w_mix_out, preferred_element_type=jnp.float32)
    after_mix = (residual + normalize(mix_out, gain_mix_post)).astype(jnp.bfloat16)
    after_float = after_mix.astype(jnp.float32)
    expert_in = normalize(after_float, gain_ffn).astype(jnp.bfloat16)
    own_routes = lax.dynamic_slice_in_dim(routing, device_index * seq_rows, seq_rows, 0)
    route_weight = route_weights(expert_in, w_router, own_routes)
    flat_routes = own_routes.reshape(-1)
    flat_hot = (flat_routes[:, None] == jnp.arange(experts, dtype=jnp.int32)[None, :]).astype(
        jnp.int32
    )
    slot_index = jnp.sum((jnp.cumsum(flat_hot, axis=0) - 1) * flat_hot, axis=1)
    position = (flat_routes * capacity + slot_index).reshape(seq_rows, top_count)
    placed = position[:, :, None] == jnp.arange(experts * capacity, dtype=jnp.int32)
    dispatch = jnp.any(placed, axis=1).astype(jnp.bfloat16)
    outgoing = jnp.einsum(
        "rp,rd->pd", dispatch, expert_in, preferred_element_type=jnp.float32
    ).astype(jnp.bfloat16)
    arrived = dispatch_rows(outgoing.reshape(experts, capacity, model_width), group_size)
    computed = expert_quarter(
        arrived.reshape(-1, model_width), w_expert_gate, w_expert_up, w_expert_down
    )
    returned = return_rows(computed.reshape(arrived.shape))
    summed = returned.astype(jnp.float32).reshape(experts * capacity, model_width)
    combine = jnp.sum(jnp.where(placed, route_weight[:, :, None], 0.0), axis=1)
    expert_sum = jnp.dot(combine, summed, precision=lax.Precision.HIGHEST)
    mixed = (after_float + normalize(expert_sum, gain_ffn_post)).astype(jnp.bfloat16)
    return (mixed, cells_next, norm_next, stab_next)


def solution(mesh):
    return jax.shard_map(
        body,
        mesh=mesh,
        in_specs=(
            P("ep", None),
            P(),
            P(),
            P(),
            P(),
            P(),
            P(),
            P(),
            P(),
            P("ep", None, None, None),
            P("ep", None, None),
            P("ep", None),
            P(),
            P(),
            P(),
            P(),
            P(),
            P("ep", None, None),
            P("ep", None, None),
            P("ep", None, None),
            P(),
        ),
        out_specs=(P("ep", None), P("ep", None, None, None), P("ep", None, None), P("ep", None)),
        check_vma=False,
    )
```

```python
import functools

import jax
import jax.numpy as jnp
from jax import lax
from jax.experimental import pallas as pl
from jax.experimental.pallas import tpu as pltpu
from jax.sharding import PartitionSpec as P

epsilon = 1e-06


def normalize(values, gain):
    return values * lax.rsqrt(jnp.mean(values * values, axis=-1, keepdims=True) + epsilon) * gain


def rounded(values):
    return lax.optimization_barrier(values.astype(jnp.bfloat16)).astype(jnp.float32)


def cell_kernel(keep, cells, queries, keys, values, cells_next, numerator):
    block, heads, key_size, value_size = cells.shape
    first = pl.program_id(0) * block
    for row in range(block):
        for head in range(heads):
            span = slice(head * key_size, (head + 1) * key_size)
            key_column = keys[0, span, row : row + 1]
            query_column = queries[0, span, row : row + 1]
            value_row = values[row, head : head + 1, :]
            updated = keep[first + row, head] * cells[row, head] + key_column * value_row
            cells_next[row, head] = updated
            numerator[row, head : head + 1, :] = jnp.sum(
                query_column * updated, axis=0, keepdims=True
            )


def update_cells(keep, cells, queries, keys, values):
    rows, heads, key_size, value_size = cells.shape
    block = next(size for size in (4, 2, 1) if rows % size == 0)

    def columns(array):
        flat = array.reshape(rows // block, block, heads * key_size)
        return jnp.swapaxes(flat, 1, 2)

    cell_spec = pl.BlockSpec((block, heads, key_size, value_size), lambda i: (i, 0, 0, 0))
    column_spec = pl.BlockSpec((1, heads * key_size, block), lambda i: (i, 0, 0))
    value_spec = pl.BlockSpec((block, heads, value_size), lambda i: (i, 0, 0))
    return pl.pallas_call(
        cell_kernel,
        grid=(rows // block,),
        out_shape=(
            jax.ShapeDtypeStruct(cells.shape, jnp.float32),
            jax.ShapeDtypeStruct(values.shape, jnp.float32),
        ),
        in_specs=[
            pl.BlockSpec(memory_space=pltpu.SMEM),
            cell_spec,
            column_spec,
            column_spec,
            value_spec,
        ],
        out_specs=(cell_spec, value_spec),
        compiler_params=pltpu.CompilerParams(vmem_limit_bytes=56 * 2**20),
        name="update_cells",
    )(keep, cells, columns(queries), columns(keys), values)


def cell_step(
    normed,
    w_query,
    w_key,
    w_value,
    w_input_gate,
    w_forget_gate,
    bias_input,
    bias_forget,
    memory_cells,
    normalizer,
    stabilizer,
):
    row_count, heads, key_size, value_size = memory_cells.shape
    query_rows = rounded(jnp.dot(normed, w_query, preferred_element_type=jnp.float32))
    query_rows = query_rows.reshape(row_count, heads, key_size) * key_size ** (-0.5)
    key_rows = rounded(jnp.dot(normed, w_key, preferred_element_type=jnp.float32)).reshape(
        row_count, heads, key_size
    )
    value_rows = rounded(jnp.dot(normed, w_value, preferred_element_type=jnp.float32)).reshape(
        row_count, heads, value_size
    )
    input_gate = jnp.dot(normed, w_input_gate, preferred_element_type=jnp.float32) + bias_input
    log_forget = jax.nn.log_sigmoid(
        jnp.dot(normed, w_forget_gate, preferred_element_type=jnp.float32) + bias_forget
    )
    carried = log_forget + stabilizer
    stab_next = jnp.maximum(carried, input_gate)
    keep_weight = jnp.exp(carried - stab_next)
    write_weight = jnp.exp(input_gate - stab_next)
    scaled_keys = write_weight[:, :, None] * key_rows
    norm_next = keep_weight[:, :, None] * normalizer + scaled_keys
    cells_next, numerator = update_cells(
        keep_weight, memory_cells, query_rows, scaled_keys, value_rows
    )
    denominator = jnp.einsum("bhd,bhd->bh", query_rows, norm_next, precision=lax.Precision.HIGHEST)
    denominator = jnp.maximum(jnp.abs(denominator), jnp.exp(-stab_next))
    cell_out = (
        (numerator / denominator[:, :, None])
        .reshape(row_count, heads * value_size)
        .astype(jnp.bfloat16)
    )
    return (cell_out, cells_next, norm_next, stab_next)


def route_weights(rows_in, w_router, routes):
    logits = jnp.dot(rows_in, w_router, preferred_element_type=jnp.float32)
    onehot = routes[:, :, None] == jnp.arange(w_router.shape[1], dtype=jnp.int32)[None, None, :]
    chosen = jnp.sum(jnp.where(onehot, logits[:, None, :], 0.0), axis=-1)
    return jax.nn.sigmoid(chosen - chosen[:, ::-1])


VMEM = pl.BlockSpec(memory_space=pltpu.VMEM)


def remote_copy(src, dst, sems, kind, step, target):
    return pltpu.make_async_remote_copy(
        src_ref=src,
        dst_ref=dst,
        send_sem=sems[0].at[kind, step],
        recv_sem=sems[1].at[kind, step],
        device_id=(target,),
        device_id_type=pl.DeviceIdType.MESH,
    )


def places(group_size):
    me = lax.axis_index("ep")
    own = lax.div(me, group_size)
    member = lax.rem(me, group_size)
    core_mate = member + 1 - 2 * lax.rem(member, 2)
    chip_mate = lax.rem(member + 2, group_size)
    far_mate = lax.rem(core_mate + 2, group_size)
    return own, member, core_mate, chip_mate, far_mate


def paired(own, step):
    other = own
    bit = 1
    while bit <= step:
        if step & bit:
            other = other + bit - 2 * bit * lax.rem(lax.div(own, bit), 2)
        bit *= 2
    return other


def greet(experts, group_size):
    own, member, core_mate, chip_mate, _ = places(group_size)
    barrier = pltpu.get_barrier_semaphore()

    def signal(target):
        pl.semaphore_signal(
            barrier, inc=1, device_id=(target,), device_id_type=pl.DeviceIdType.MESH
        )

    for step in range(1, experts):
        signal(paired(own, step) * group_size + member)
    signal(own * group_size + core_mate)
    signal(own * group_size + chip_mate)
    pl.semaphore_wait(barrier, experts + 1)


def dispatch_kernel(experts, group_size, outgoing, arrived, send_sems, recv_sems):
    own, member, core_mate, chip_mate, _ = places(group_size)
    sems = (send_sems, recv_sems)
    greet(experts, group_size)

    def direct(step):
        target = paired(own, step)
        return remote_copy(
            outgoing.at[target],
            arrived.at[own, member],
            sems,
            0,
            step,
            target * group_size + member,
        )

    def forward(step, kind):
        source = paired(own, step)
        mate = core_mate if kind != 2 else chip_mate
        row = member if kind != 3 else chip_mate
        src = arrived.at[source, row]
        if step == 0 and kind != 3:
            src = outgoing.at[own]
        return remote_copy(
            src, arrived.at[source, row], sems, kind, step, own * group_size + mate
        )

    for step in range(1, experts):
        direct(step).start()
    forward(0, 2).start()
    forward(0, 1).start()
    arrived[own, member] = outgoing[own]
    for step in range(1, experts):
        direct(step).wait_recv()
        forward(step, 2).start()
        forward(step, 1).start()
        forward(step - 1, 2).wait_recv()
        forward(step - 1, 3).start()
    forward(experts - 1, 2).wait_recv()
    forward(experts - 1, 3).start()
    for step in range(experts):
        if step:
            direct(step).wait_send()
        forward(step, 2).wait_send()
        forward(step, 1).wait()
        forward(step, 3).wait()


def expert_kernel(rows_in, gate_w, up_w, down_w, result):
    rows = rows_in.shape[0]
    pieces = 2 if rows % 512 == 0 else 1
    for piece in range(pieces):
        span = slice(piece * rows // pieces, (piece + 1) * rows // pieces)
        block = rows_in[span, :]
        gate_part = jnp.dot(block, gate_w[0], preferred_element_type=jnp.float32)
        up_part = jnp.dot(block, up_w[0], preferred_element_type=jnp.float32)
        hidden = (jax.nn.silu(gate_part) * up_part).astype(rows_in.dtype)
        result[span, :] = jnp.dot(
            hidden, down_w[0], preferred_element_type=jnp.float32
        ).astype(result.dtype)


def expert_quarter(rows_in, gate_w, up_w, down_w):
    return pl.pallas_call(
        expert_kernel,
        out_shape=jax.ShapeDtypeStruct(rows_in.shape, rows_in.dtype),
        in_specs=[VMEM] * 4,
        out_specs=VMEM,
        compiler_params=pltpu.CompilerParams(vmem_limit_bytes=24 * 2**20),
        name="expert_quarter",
    )(rows_in, gate_w, up_w, down_w)


def dispatch_rows(outgoing, group_size):
    experts, capacity, width = outgoing.shape
    return pl.pallas_call(
        functools.partial(dispatch_kernel, experts, group_size),
        out_shape=jax.ShapeDtypeStruct((experts, group_size, capacity, width), outgoing.dtype),
        in_specs=[VMEM],
        out_specs=VMEM,
        scratch_shapes=[
            pltpu.SemaphoreType.DMA((4, experts)),
            pltpu.SemaphoreType.DMA((4, experts)),
        ],
        compiler_params=pltpu.CompilerParams(
            collective_id=0, has_side_effects=True, vmem_limit_bytes=12 * 2**20
        ),
        name="dispatch_rows",
    )(outgoing)


def return_kernel(
    experts,
    group_size,
    computed,
    returned,
    core_in,
    chip_out,
    chip_in,
    final_out,
    send_sems,
    recv_sems,
):
    own, member, core_mate, chip_mate, far_mate = places(group_size)
    sems = (send_sems, recv_sems)
    greet(experts, group_size)

    def source_of(step):
        return paired(own, step)

    def to_core(step, kind):
        row = core_mate if kind == 0 else far_mate
        return remote_copy(
            computed.at[source_of(step), row],
            core_in.at[kind, step],
            sems,
            kind,
            step,
            own * group_size + core_mate,
        )

    def to_chip(step):
        return remote_copy(
            chip_out.at[step], chip_in.at[step], sems, 2, step, own * group_size + chip_mate
        )

    def to_source(step):
        target = source_of(step)
        return remote_copy(
            final_out.at[step], returned.at[own], sems, 3, step, target * group_size + member
        )

    def wide(values):
        return values.astype(jnp.float32)

    order = list(range(experts - 1, -1, -1))
    for step in order:
        to_core(step, 1).start()
        to_core(step, 0).start()
    before = None
    for step in order:
        to_core(step, 1).wait_recv()
        total = wide(computed[source_of(step), chip_mate]) + wide(core_in[1, step])
        chip_out[step] = total.astype(chip_out.dtype)
        if before is not None:
            to_chip(before).start()
        before = step
    for step in order:
        to_core(step, 0).wait_recv()
        if before is not None:
            to_chip(before).start()
            before = None
    for step in order:
        to_chip(step).wait_recv()
        total = wide(computed[source_of(step), member]) + wide(core_in[0, step])
        total = (total + wide(chip_in[step])).astype(final_out.dtype)
        if step:
            final_out[step] = total
        else:
            returned[own] = total
        if before is not None:
            to_source(before).start()
        before = step if step else None
    for step in range(experts):
        to_core(step, 0).wait_send()
        to_core(step, 1).wait_send()
        to_chip(step).wait_send()
        if step:
            to_source(step).wait()


def return_rows(computed):
    experts, group_size, capacity, width = computed.shape
    chunk = (experts, capacity, width)
    return pl.pallas_call(
        functools.partial(return_kernel, experts, group_size),
        out_shape=jax.ShapeDtypeStruct(chunk, computed.dtype),
        in_specs=[VMEM],
        out_specs=VMEM,
        scratch_shapes=[
            pltpu.VMEM((2,) + chunk, computed.dtype),
            pltpu.VMEM(chunk, computed.dtype),
            pltpu.VMEM(chunk, computed.dtype),
            pltpu.VMEM(chunk, computed.dtype),
            pltpu.SemaphoreType.DMA((4, experts)),
            pltpu.SemaphoreType.DMA((4, experts)),
        ],
        compiler_params=pltpu.CompilerParams(
            collective_id=1, has_side_effects=True, vmem_limit_bytes=16 * 2**20
        ),
        name="return_rows",
    )(computed)


def body(
    tokens,
    gain_mix,
    w_query,
    w_key,
    w_value,
    w_input_gate,
    w_forget_gate,
    bias_input,
    bias_forget,
    memory_cells,
    normalizer,
    stabilizer,
    w_mix_out,
    gain_mix_post,
    gain_ffn,
    w_router,
    routing,
    w_expert_gate,
    w_expert_up,
    w_expert_down,
    gain_ffn_post,
):
    devices = lax.axis_size("ep")
    device_index = lax.axis_index("ep")
    seq_rows = tokens.shape[0]
    model_width = tokens.shape[1]
    experts = w_router.shape[1]
    group_size = devices // experts
    top_count = routing.shape[1]
    capacity = max(2, seq_rows * top_count * 2 // experts)
    residual = tokens.astype(jnp.float32)
    normed = normalize(residual, gain_mix).astype(jnp.bfloat16)
    cell_out, cells_next, norm_next, stab_next = cell_step(
        normed,
        w_query,
        w_key,
        w_value,
        w_input_gate,
        w_forget_gate,
        bias_input,
        bias_forget,
        memory_cells,
        normalizer,
        stabilizer,
    )
    mix_out = jnp.dot(cell_out, w_mix_out, preferred_element_type=jnp.float32)
    after_mix = (residual + normalize(mix_out, gain_mix_post)).astype(jnp.bfloat16)
    after_float = after_mix.astype(jnp.float32)
    expert_in = normalize(after_float, gain_ffn).astype(jnp.bfloat16)
    own_routes = lax.dynamic_slice_in_dim(routing, device_index * seq_rows, seq_rows, 0)
    route_weight = route_weights(expert_in, w_router, own_routes)
    flat_routes = own_routes.reshape(-1)
    flat_hot = (flat_routes[:, None] == jnp.arange(experts, dtype=jnp.int32)[None, :]).astype(
        jnp.int32
    )
    slot_index = jnp.sum((jnp.cumsum(flat_hot, axis=0) - 1) * flat_hot, axis=1)
    position = (flat_routes * capacity + slot_index).reshape(seq_rows, top_count)
    placed = position[:, :, None] == jnp.arange(experts * capacity, dtype=jnp.int32)
    dispatch = jnp.any(placed, axis=1).astype(jnp.bfloat16)
    outgoing = jnp.einsum(
        "rp,rd->pd", dispatch, expert_in, preferred_element_type=jnp.float32
    ).astype(jnp.bfloat16)
    arrived = dispatch_rows(outgoing.reshape(experts, capacity, model_width), group_size)
    computed = expert_quarter(
        arrived.reshape(-1, model_width), w_expert_gate, w_expert_up, w_expert_down
    )
    returned = return_rows(computed.reshape(arrived.shape))
    summed = returned.astype(jnp.float32).reshape(experts * capacity, model_width)
    combine = jnp.sum(jnp.where(placed, route_weight[:, :, None], 0.0), axis=1)
    expert_sum = jnp.dot(combine, summed, precision=lax.Precision.HIGHEST)
    mixed = (after_float + normalize(expert_sum, gain_ffn_post)).astype(jnp.bfloat16)
    return (mixed, cells_next, norm_next, stab_next)


def solution(mesh):
    return jax.shard_map(
        body,
        mesh=mesh,
        in_specs=(
            P("ep", None),
            P(),
            P(),
            P(),
            P(),
            P(),
            P(),
            P(),
            P(),
            P("ep", None, None, None),
            P("ep", None, None),
            P("ep", None),
            P(),
            P(),
            P(),
            P(),
            P(),
            P("ep", None, None),
            P("ep", None, None),
            P("ep", None, None),
            P(),
        ),
        out_specs=(P("ep", None), P("ep", None, None, None), P("ep", None, None), P("ep", None)),
        check_vma=False,
    )
```
